32 devices in a mesh: grp: 2 (over y), fs: 4 (over z), tp: 4 (over x, core).
Axes of the slice: x: 2, y: 2, z: 4, core: 2. Of those that a mesh axis runs over, the one named last changes fastest.
Arguments:
- tokens: bfloat16 [8192, 2048], P(('grp', 'fs')), parts along dimension 0, may hold values from -6 to 6
- mixer_gain: float32 [2048], replicated, may hold values from 0.1 to 1.9
- outer_weight: float32 [2048, 2048], P('fs', 'tp'), may hold values from -0.125 to 0.125
- inner_weight: float32 [2048, 2048], P('fs', 'tp'), may hold values from -0.125 to 0.125
- value_weight: float32 [2048, 2048], P('fs', 'tp'), may hold values from -0.125 to 0.125
- filter_taps: float32 [3, 2048], P(None, 'tp'), may hold values from -3.5 to 3.5
- mixer_weight: float32 [2048, 2048], P('tp', 'fs'), may hold values from -0.125 to 0.125
- outer_scale: float32 [4, 512], P('tp', 'fs'), may hold values from 0.5 to 2
- inner_scale: float32 [4, 512], P('tp', 'fs'), may hold values from 0.5 to 2
- value_scale: float32 [4, 512], P('tp', 'fs'), may hold values from 0.5 to 2
- mixer_scale: float32 [1, 2048], P(None, 'fs'), may hold values from 0.5 to 2
Outputs:
- layer_out: bfloat16 [8192, 2048], P(('grp', 'fs', 'tp')), parts along dimension 0
The draws below stay inside these ranges and needn't reach their ends.
There are 2 independent parts, one for each index of `grp`. The reference program is written for one: setup_inputs(seed, part) draws one part's arguments, and reference() takes and returns one part's arrays. A program takes and returns all parts, laid end to end along the dimension named above; an argument that names none is the same for every part. Nothing has to cross between parts.
All inputs are finite; a program needn't handle non-finite values.
Results may differ from the reference program's by a relative error of at most 0.014.
Values may be sent and summed in bfloat16 or wider, within the bound.
A program may use at most 64 MiB of HBM per device.

```python
import math
import jax
import jax.numpy as jnp
from jax import lax

D = 2048
DC = 2048
SEQ_LEN = 1024
TOKENS = 4096
N_FS = 4
N_TP = 4


def levels(key, dims, shards, smallest, top_value):
    factor_of = 1.0
    for axis_at, blocks in shards:
        heights = jax.random.uniform(jax.random.fold_in(jax.random.fold_in(key, 6), axis_at), (blocks,), jnp.float32, smallest / len(shards), top_value / len(shards))
        factor_of = factor_of * jnp.repeat(jnp.exp(heights), dims[axis_at] // blocks).reshape((-1,) + (1,) * (len(dims) - 1 - axis_at))
    return factor_of


def centred(stream_key, dims, scale, reach, cuts=(), held_as=jnp.bfloat16):
    drawn = scale * jax.random.normal(stream_key, dims, jnp.float32)
    if cuts:
        drawn = drawn * levels(stream_key, dims, cuts, -0.22, 0.18)
    return jnp.clip(drawn, -reach, reach).astype(held_as)


def setup_inputs(seed: int = 0, part: int = 0) -> dict:
    streams_of = jax.random.split(jax.random.key(seed), 12)
    own_keys = jax.random.split(jax.random.fold_in(streams_of[11], part), 12)
    tokens = centred(own_keys[0], (TOKENS, D), 1.0, 6.0, ((0, 4),))
    mixer_gain = jnp.clip(1.0 + 0.18 * jax.random.normal(streams_of[1], (D,), jnp.float32), 0.1, 1.9)
    outer_weight = centred(streams_of[2], (D, DC), D ** -0.5, 0.125, ((0, 4), (1, 4)), jnp.float32)
    inner_weight = centred(streams_of[3], (D, DC), D ** -0.5, 0.125, ((0, 4), (1, 4)), jnp.float32)
    value_weight = centred(streams_of[4], (D, DC), D ** -0.5, 0.125, ((0, 4), (1, 4)), jnp.float32)
    filter_taps = centred(streams_of[5], (3, DC), 3 ** -0.5, 3.5, ((1, 4),), jnp.float32)
    mixer_weight = centred(streams_of[6], (DC, D), DC ** -0.5, 0.125, ((0, 4), (1, 4)), jnp.float32)
    outer_scale = jnp.clip(jnp.exp(math.log(2.0) - 1.3862944 * jax.random.uniform(streams_of[7], (N_TP, DC // N_TP), jnp.float32) ** levels(streams_of[7], (N_TP, DC // N_TP), ((0, 4), (1, 4)), -0.2, 0.2)), 0.5, 2.0)
    inner_scale = jnp.clip(jnp.exp(math.log(2.0) - 1.3862944 * jax.random.uniform(streams_of[8], (N_TP, DC // N_TP), jnp.float32) ** levels(streams_of[8], (N_TP, DC // N_TP), ((0, 4), (1, 4)), -0.2, 0.2)), 0.5, 2.0)
    value_scale = jnp.clip(jnp.exp(math.log(2.0) - 1.3862944 * jax.random.uniform(streams_of[9], (N_TP, DC // N_TP), jnp.float32) ** levels(streams_of[9], (N_TP, DC // N_TP), ((0, 4), (1, 4)), -0.2, 0.2)), 0.5, 2.0)
    mixer_scale = jnp.clip(jnp.exp(math.log(2.0) - 1.3862944 * jax.random.uniform(streams_of[10], (1, D), jnp.float32) ** levels(streams_of[10], (1, D), ((1, 4),), -0.2, 0.2)), 0.5, 2.0)
    return dict(tokens=tokens, mixer_gain=mixer_gain, outer_weight=outer_weight, inner_weight=inner_weight, value_weight=value_weight, filter_taps=filter_taps, mixer_weight=mixer_weight, outer_scale=outer_scale, inner_scale=inner_scale, value_scale=value_scale, mixer_scale=mixer_scale)


EPS = 1e-06

def normed(rows, gain):
    values = rows.astype(jnp.float32)
    inverse = lax.rsqrt(lax.optimization_barrier(jnp.mean(values * values, axis=-1, keepdims=True)) + EPS)
    return (values * inverse * gain).astype(jnp.bfloat16)

def project(left, weight, scale):
    return jnp.dot(left, weight.astype(jnp.bfloat16), preferred_element_type=jnp.float32) * scale.reshape(-1)

def rounded(values):
    return lax.optimization_barrier(values.astype(jnp.bfloat16)).astype(jnp.float32)

def summed_blocks(hidden, weight, scale):
    width = hidden.shape[1] // N_TP
    total = jnp.zeros((hidden.shape[0], weight.shape[1]), jnp.float32)
    for index in range(N_TP):
        part = project(hidden[:, index * width:(index + 1) * width], weight[index * width:(index + 1) * width], scale)
        total = total + rounded(part)
    return total

def reference(tokens, mixer_gain, outer_weight, inner_weight, value_weight, filter_taps, mixer_weight, outer_scale, inner_scale, value_scale, mixer_scale):
    normal_rows = normed(tokens, mixer_gain)
    outer = rounded(project(normal_rows, outer_weight, outer_scale))
    inner = rounded(project(normal_rows, inner_weight, inner_scale))
    value = rounded(project(normal_rows, value_weight, value_scale))
    product = (inner * value).reshape(N_FS, SEQ_LEN, DC)
    padded = jnp.pad(product, ((0, 0), (2, 0), (0, 0)))
    filtered = filter_taps[0] * padded[:, 0:SEQ_LEN] + filter_taps[1] * padded[:, 1:SEQ_LEN + 1] + filter_taps[2] * padded[:, 2:]
    gated = (outer * filtered.reshape(TOKENS, DC)).astype(jnp.bfloat16)
    return summed_blocks(gated, mixer_weight, mixer_scale).astype(jnp.bfloat16)
```

```python
import functools

import jax
import jax.numpy as jnp
from jax import lax
from jax.experimental import pallas as pl
from jax.experimental.pallas import tpu as pltpu
from jax.sharding import PartitionSpec as P

EPS = 1e-06


def normed(rows, gain):
    values = rows.astype(jnp.float32)
    inverse = lax.rsqrt(jnp.mean(values * values, axis=-1, keepdims=True) + EPS)
    return (values * inverse * gain).astype(jnp.bfloat16)


def rounded(values):
    return lax.optimization_barrier(values.astype(jnp.bfloat16)).astype(jnp.float32)


def add_rows(left, piece):
    return jnp.dot(left, piece, preferred_element_type=jnp.float32)


def per_device(
    tokens,
    mixer_gain,
    outer_weight,
    inner_weight,
    value_weight,
    filter_taps,
    mixer_weight,
    outer_scale,
    inner_scale,
    value_scale,
    mixer_scale,
):
    gathered = (
        lax.all_gather(outer_scale, "fs", axis=1, tiled=True),
        lax.all_gather(inner_scale, "fs", axis=1, tiled=True),
        lax.all_gather(value_scale, "fs", axis=1, tiled=True),
        lax.all_gather(mixer_scale, "fs", axis=1, tiled=True),
    )
    outer_col, inner_col, value_col, mixer_col = [piece.reshape(-1) for piece in gathered]
    seq_rows = tokens.shape[0]
    normal_rows = normed(tokens, mixer_gain)

    def fold_one(piece):
        return add_rows(normal_rows, piece)

    outer_sum = fold_one(
        lax.all_gather(outer_weight.astype(jnp.bfloat16), "fs", axis=0, tiled=True)
    )
    inner_sum = fold_one(
        lax.all_gather(inner_weight.astype(jnp.bfloat16), "fs", axis=0, tiled=True)
    )
    value_sum = fold_one(
        lax.all_gather(value_weight.astype(jnp.bfloat16), "fs", axis=0, tiled=True)
    )
    outer = rounded(outer_sum * outer_col)
    inner = rounded(inner_sum * inner_col)
    value = rounded(value_sum * value_col)
    padded = jnp.pad(inner * value, ((2, 0), (0, 0)))
    filtered = (
        filter_taps[0] * padded[0:seq_rows]
        + filter_taps[1] * padded[1 : seq_rows + 1]
        + filter_taps[2] * padded[2:]
    )
    gated = (outer * filtered).astype(jnp.bfloat16)
    mixer_full = lax.all_gather(mixer_weight.astype(jnp.bfloat16), "fs", axis=1, tiled=True)
    return lax.psum_scatter(
        (jnp.dot(gated, mixer_full, preferred_element_type=jnp.float32) * mixer_col).astype(
            jnp.bfloat16
        ),
        "tp",
        scatter_dimension=0,
        tiled=True,
    )


MESH = pl.DeviceIdType.MESH
MATRICES = 3
EARLY = 2


def mixer_kernel(
    n,
    tokens_hbm,
    gain_ref,
    w0_hbm,
    w1_hbm,
    w2_hbm,
    taps_ref,
    w3_hbm,
    s0_ref,
    s1_ref,
    s2_ref,
    s3_ref,
    out_ref,
    toks,
    rows,
    stage,
    held,
    mix,
    scales,
    acc,
    product,
    gated,
    gates_in,
    mixed,
    load_sem,
    zl_sem,
    zr_sem,
    zin_sem,
    yout_sem,
    yin_sem,
    dout_sem,
    din_sem,
    sout_sem,
    sin_sem,
    xout_sem,
    xin_sem,
    cout_sem,
    cin_sem,
    rout_sem,
    rin_sem,
    gout_sem,
    gin_sem,
):
    z = lax.axis_index("fs")
    y = lax.axis_index("grp")
    t = lax.axis_index("tp")
    ntp = 4
    block = stage.shape[1]
    half = block // 2
    seq = rows.shape[0]
    tile = seq // ntp
    q = s0_ref.shape[1]
    pieces = EARLY + n
    partner = t + 1 - 2 * lax.rem(t, 2)
    across = lax.rem(t + 2, ntp)
    corner = lax.rem(partner + 2, ntp)
    peers = (partner, across, corner)
    weights = (w0_hbm, w1_hbm, w2_hbm, w3_hbm)

    loads = [
        pltpu.make_async_copy(weights[m], stage.at[m], load_sem.at[m]) for m in range(MATRICES + 1)
    ]
    token_load = pltpu.make_async_copy(tokens_hbm, toks, load_sem.at[MATRICES + 1])
    loads[MATRICES].start()
    for m in range(MATRICES):
        loads[m].start()
    token_load.start()

    barrier = pltpu.get_barrier_semaphore()
    for d in range(1, n):
        pl.semaphore_signal(
            barrier, inc=1, device_id={"fs": lax.rem(z + d, n)}, device_id_type=MESH
        )
    for d in range(1, ntp):
        pl.semaphore_signal(
            barrier, inc=1, device_id={"tp": lax.rem(t + d, ntp)}, device_id_type=MESH
        )
    pl.semaphore_signal(barrier, inc=1, device_id={"grp": 1 - y}, device_id_type=MESH)

    scales[z, :, 0:q] = s0_ref[...]
    scales[z, :, q : 2 * q] = s1_ref[...]
    scales[z, :, 2 * q : 3 * q] = s2_ref[...]
    scales[z, :, 3 * q :] = s3_ref[...]

    def piece(p, b, side):
        if p < EARLY:
            return mix.at[b, EARLY * side + p, t]
        first = pl.multiple_of(b * block + side * half, half)
        return held.at[p - EARLY, pl.ds(first, half), :]

    def remote(ref, send, recv, target):
        return pltpu.make_async_remote_copy(
            src_ref=ref,
            dst_ref=ref,
            send_sem=send,
            recv_sem=recv,
            device_id=target,
            device_id_type=MESH,
        )

    def to_left(p, b):
        return remote(piece(p, b, y), zl_sem.at[p, b], zin_sem.at[p, b], {"fs": z - 1})

    def to_right(p, b):
        return remote(piece(p, b, y), zr_sem.at[p, b], zin_sem.at[p, b], {"fs": z + 1})

    def to_twin(p, b):
        return remote(piece(p, b, y), yout_sem.at[p, b], yin_sem.at[p, b], {"grp": 1 - y})

    def from_twin(p, b):
        return remote(piece(p, b, 1 - y), yout_sem.at[p, b], yin_sem.at[p, b], {"grp": 1 - y})

    inward = jnp.where(z == 0, 1, n - 2)

    def second_half(p, b):
        return remote(piece(p, b, 1 - y), dout_sem.at[p], din_sem.at[p], {"fs": inward})

    def direct(b):
        return ((z == 1) & (b == 0)) | ((z == n - 2) & (b == n - 1))

    at_end = (z == 0) | (z == n - 1)

    def scale_copy(d):
        return remote(scales.at[z], sout_sem.at[d], sin_sem.at[z], {"fs": lax.rem(z + d, n)})

    def scale_arrival(d):
        source = lax.rem(z + d, n)
        return remote(scales.at[source], sout_sem.at[d], sin_sem.at[source], {"fs": source})

    def send_own(p):
        @pl.when(z >= 1)
        def _():
            to_left(p, z).start()

        @pl.when(z <= n - 2)
        def _():
            to_right(p, z).start()

        @pl.when(at_end)
        def _():
            second_half(p, z).start()

    def relay(p, s):
        from_right, from_left = z + 1 + s, z - 1 - s

        @pl.when(from_right <= n - 1)
        def _():
            to_left(p, from_right).wait_recv()

            @pl.when(z >= 1)
            def _():
                to_left(p, from_right).start()

            @pl.when(jnp.logical_not(direct(from_right)))
            def _():
                to_twin(p, from_right).start()

        @pl.when(from_left >= 0)
        def _():
            to_right(p, from_left).wait_recv()

            @pl.when(z <= n - 2)
            def _():
                to_right(p, from_left).start()

            @pl.when(jnp.logical_not(direct(from_left)))
            def _():
                to_twin(p, from_left).start()

    def second_arrived(p, b):
        @pl.when(direct(b))
        def _():
            second_half(p, b).wait_recv()

        @pl.when(jnp.logical_not(direct(b)))
        def _():
            from_twin(p, b).wait_recv()

    def each_block(s, act):
        @pl.loop(0, 2)
        def _(side):
            b = z + (1 + s) * (1 - 2 * side)

            @pl.when((b >= 0) & (b <= n - 1))
            def _():
                act(b)

    def across_copy(b):
        return remote(mix.at[b, :, t], xout_sem.at[b], xin_sem.at[b], {"tp": across})

    def across_arrival(b):
        return remote(mix.at[b, :, across], xout_sem.at[b], xin_sem.at[b], {"tp": across})

    def core_copy(b):
        return remote(mix.at[b, :, t], cout_sem.at[b], cin_sem.at[b], {"tp": partner})

    def core_arrival(b):
        return remote(mix.at[b, :, partner], cout_sem.at[b], cin_sem.at[b], {"tp": partner})

    def core_relay(b):
        return remote(mix.at[b, :, across], rout_sem.at[b], rin_sem.at[b], {"tp": partner})

    def core_relay_arrival(b):
        return remote(mix.at[b, :, corner], rout_sem.at[b], rin_sem.at[b], {"tp": partner})

    def spread(b):
        across_copy(b).start()
        core_copy(b).start()

    def spread_arrived(s):
        def act(b):
            for p in range(EARLY):
                second_arrived(p, b)
            spread(b)

        each_block(s, act)

    def pass_on(b):
        across_arrival(b).wait_recv()
        core_relay(b).start()

    def multiply(c, b, first_time=False):
        at = pl.ds(pl.multiple_of(b * block, block), block)
        for i in range(2):
            r = slice(i * seq // 2, (i + 1) * seq // 2)
            part = jnp.dot(rows[r, at], held[c, at, :], preferred_element_type=jnp.float32)
            acc[c, r, :] = part if first_time else acc[c, r, :] + part

    def multiply_arrived(c, s):
        def act(b):
            second_arrived(EARLY + c, b)
            multiply(c, b)

        each_block(s, act)

    def gate_copy(c, k):
        return pltpu.make_async_remote_copy(
            src_ref=gated.at[c, pl.ds(pl.multiple_of(peers[k] * tile, tile), tile), :],
            dst_ref=gates_in.at[c, t],
            send_sem=gout_sem.at[c, k],
            recv_sem=gin_sem.at[c, k],
            device_id={"tp": peers[k]},
            device_id_type=MESH,
        )

    def gate_arrival(c, k):
        return remote(gates_in.at[c, peers[k]], gout_sem.at[c, k], gin_sem.at[c, k], {"tp": peers[k]})

    def gate(c):
        col = scales[c, :, 0 : 3 * q]
        lanes = slice(c * q, (c + 1) * q)

        def scaled(m):
            part = acc[c, :, m * q : (m + 1) * q] * col[:, m * q : (m + 1) * q]
            return part.astype(jnp.bfloat16).astype(jnp.float32)

        product[8:, :] = scaled(1) * scaled(2)
        filtered = (
            taps_ref[0:1, lanes] * product[6 : 6 + seq, :]
            + taps_ref[1:2, lanes] * product[7 : 7 + seq, :]
            + taps_ref[2:3, lanes] * product[8 : 8 + seq, :]
        )
        gated[c] = (scaled(0) * filtered).astype(jnp.bfloat16)
        for k in (2, 1, 0):
            gate_copy(c, k).start()
        gates_in[c, t] = gated[c, pl.ds(pl.multiple_of(t * tile, tile), tile), :]

    def gates_arrived(c):
        for k in range(ntp - 1):
            gate_arrival(c, k).wait_recv()

    def mix_chunks(first, last, final):
        count = last - first
        left = jnp.concatenate(
            [gates_in[c, k] for c in range(first, last) for k in range(ntp)], axis=1
        )
        for b in range(n):
            cols = slice(b * block, (b + 1) * block)
            right = mix[b, first:last].reshape(count * ntp * q, block)
            part = jnp.dot(left, right, preferred_element_type=jnp.float32)
            if final:
                out_ref[:, cols] = ((mixed[:, cols] + part) * scales[b, :, 3 * q :]).astype(
                    jnp.bfloat16
                )
            else:
                mixed[:, cols] = part

    def mix_in():
        @pl.loop(0, n)
        def _(b):
            core_arrival(b).wait_recv()
            core_relay_arrival(b).wait_recv()

    strip = seq // 8

    def normalise(i):
        at = slice(i * strip, (i + 1) * strip)
        rows[at, :] = normed(toks[at, :], gain_ref[...])

    loads[MATRICES].wait()
    for c in range(n):
        mix[z, c, t] = stage[MATRICES, c * q : (c + 1) * q, :].astype(jnp.bfloat16)
    pl.semaphore_wait(barrier, n - 1 + ntp - 1 + 1)
    for p in range(EARLY):
        send_own(p)
    for d in range(1, n):
        scale_copy(d).start()
    spread(z)
    for m in range(MATRICES):
        loads[m].wait()
        for c in range(n):
            held[c, pl.ds(pl.multiple_of(z * block, block), block), m * q : (m + 1) * q] = stage[
                m, :, c * q : (c + 1) * q
            ].astype(jnp.bfloat16)
    product[0:8, :] = jnp.zeros((8, q), jnp.float32)

    @pl.when(at_end)
    def _():
        for p in range(EARLY, pieces):
            send_own(p)

    def send_own_inside(p):
        @pl.when(jnp.logical_not(at_end))
        def _():
            send_own(p)

    token_load.wait()

    def own_part(c):
        multiply(c, z, True)

    def scales_in():
        for d in range(1, n):
            scale_arrival(d).wait_recv()

    part = functools.partial
    hops = n - 1
    work = {k: [] for k in range(pieces * hops)}
    for i in range(8):
        work[i // 2].append(part(normalise, i))
    for c in range(n):
        work[4 + c // 2].append(part(own_part, c))
    for s in range(hops):
        work[hops * EARLY - 1 + s].append(part(spread_arrived, s))
    work[7].append(scales_in)
    for c in range(n):
        for s in range(hops):
            at = (EARLY + c) * hops + s + 1
            if at in work:
                work[at].append(part(multiply_arrived, c, s))
                if s == hops - 1:
                    work[at].append(part(gate, c))
    work[9].append(lambda: pass_on(z))
    work[12].append(lambda: each_block(0, pass_on))
    work[14].append(lambda: each_block(1, pass_on))
    work[15].append(lambda: each_block(2, pass_on))
    work[16] += [mix_in, part(gates_arrived, 0), part(gates_arrived, 1), part(mix_chunks, 0, 2, False)]

    for k in range(pieces * hops):
        p, s = divmod(k, hops)
        relay(p, s)
        if s == n - 3 and p + 1 < pieces and p + 1 >= EARLY:
            send_own_inside(p + 1)
        for task in work[k]:
            task()
    multiply_arrived(n - 1, hops - 1)
    gate(n - 1)
    gates_arrived(n - 2)
    gates_arrived(n - 1)
    mix_chunks(n - 2, n, True)

    for d in range(1, n):
        scale_copy(d).wait_send()
    for c in range(n):
        for k in range(ntp - 1):
            gate_copy(c, k).wait_send()

    @pl.loop(0, n)
    def _(b):
        across_copy(b).wait_send()
        core_copy(b).wait_send()
        core_relay(b).wait_send()

    for p in range(pieces):

        @pl.when(at_end)
        def _():
            second_half(p, z).wait_send()

        @pl.loop(0, n)
        def _(b):
            @pl.when((b >= z) & (z >= 1))
            def _():
                to_left(p, b).wait_send()

            @pl.when((b <= z) & (z <= n - 2))
            def _():
                to_right(p, b).wait_send()

            @pl.when((b != z) & jnp.logical_not(direct(b)))
            def _():
                to_twin(p, b).wait_send()


def fused_device(
    n,
    tokens,
    mixer_gain,
    outer_weight,
    inner_weight,
    value_weight,
    filter_taps,
    mixer_weight,
    outer_scale,
    inner_scale,
    value_scale,
    mixer_scale,
):
    ntp = 4
    seq, depth = tokens.shape
    block, width = outer_weight.shape
    tile = seq // ntp
    q = outer_scale.shape[1]
    pieces = EARLY + n
    whole = pl.BlockSpec(memory_space=pltpu.VMEM)
    anywhere = pl.BlockSpec(memory_space=pl.ANY)
    bf16, f32 = jnp.bfloat16, jnp.float32
    dma = pltpu.SemaphoreType.DMA
    scale_width = 3 * q + mixer_scale.shape[1]
    return pl.pallas_call(
        functools.partial(mixer_kernel, n),
        out_shape=jax.ShapeDtypeStruct((tile, n * block), bf16),
        in_specs=[
            anywhere,
            whole,
            anywhere,
            anywhere,
            anywhere,
            whole,
            anywhere,
            whole,
            whole,
            whole,
            whole,
        ],
        out_specs=whole,
        scratch_shapes=[
            pltpu.VMEM((seq, depth), bf16),
            pltpu.VMEM((seq, depth), bf16),
            pltpu.VMEM((MATRICES + 1, block, width), f32),
            pltpu.VMEM((n, depth, MATRICES * q), bf16),
            pltpu.VMEM((n, n, ntp, q, block), bf16),
            pltpu.VMEM((n, 1, scale_width), f32),
            pltpu.VMEM((n, seq, MATRICES * q), f32),
            pltpu.VMEM((seq + 8, q), f32),
            pltpu.VMEM((n, seq, q), bf16),
            pltpu.VMEM((n, ntp, tile, q), bf16),
            pltpu.VMEM((tile, n * block), f32),
            dma((MATRICES + 2,)),
            dma((pieces, n)),
            dma((pieces, n)),
            dma((pieces, n)),
            dma((pieces, n)),
            dma((pieces, n)),
            dma((pieces,)),
            dma((pieces,)),
            dma((n,)),
            dma((n,)),
            dma((n,)),
            dma((n,)),
            dma((n,)),
            dma((n,)),
            dma((n,)),
            dma((n,)),
            dma((n, ntp - 1)),
            dma((n, ntp - 1)),
        ],
        compiler_params=pltpu.CompilerParams(
            collective_id=0, has_side_effects=True, vmem_limit_bytes=60 * 2**20
        ),
    )(
        tokens,
        mixer_gain.reshape(1, -1),
        outer_weight,
        inner_weight,
        value_weight,
        filter_taps,
        mixer_weight,
        outer_scale,
        inner_scale,
        value_scale,
        mixer_scale,
    )


def choose(mesh):
    n, ntp, groups = mesh.shape["fs"], mesh.shape["tp"], mesh.shape["grp"]

    def run(*args):
        tokens, weight, mixer, scale = args[0], args[2], args[6], args[7]
        fits = (
            groups == 2
            and ntp == 4
            and n == 4
            and weight.shape == mixer.shape
            and weight.shape[0] == n * scale.shape[1]
            and scale.shape[1] % 128 == 0
            and tokens.shape[0] % 256 == 0
        )
        return fused_device(n, *args) if fits else per_device(*args)

    return run


def solution(mesh):
    in_specs = (
        P(("grp", "fs"), None),
        P(),
        P("fs", "tp"),
        P("fs", "tp"),
        P("fs", "tp"),
        P(None, "tp"),
        P("tp", "fs"),
        P("tp", "fs"),
        P("tp", "fs"),
        P("tp", "fs"),
        P(None, "fs"),
    )
    out_specs = P(("grp", "fs", "tp"), None)
    return jax.shard_map(
        choose(mesh), mesh=mesh, in_specs=in_specs, out_specs=out_specs, check_vma=False
    )
```

```python
import functools

import jax
import jax.numpy as jnp
from jax import lax
from jax.experimental import pallas as pl
from jax.experimental.pallas import tpu as pltpu
from jax.sharding import PartitionSpec as P

EPS = 1e-06


def normed(rows, gain):
    values = rows.astype(jnp.float32)
    inverse = lax.rsqrt(jnp.mean(values * values, axis=-1, keepdims=True) + EPS)
    return (values * inverse * gain).astype(jnp.bfloat16)


def rounded(values):
    return lax.optimization_barrier(values.astype(jnp.bfloat16)).astype(jnp.float32)


def add_rows(left, piece):
    return jnp.dot(left, piece, preferred_element_type=jnp.float32)


def per_device(
    tokens,
    mixer_gain,
    outer_weight,
    inner_weight,
    value_weight,
    filter_taps,
    mixer_weight,
    outer_scale,
    inner_scale,
    value_scale,
    mixer_scale,
):
    gathered = (
        lax.all_gather(outer_scale, "fs", axis=1, tiled=True),
        lax.all_gather(inner_scale, "fs", axis=1, tiled=True),
        lax.all_gather(value_scale, "fs", axis=1, tiled=True),
        lax.all_gather(mixer_scale, "fs", axis=1, tiled=True),
    )
    outer_col, inner_col, value_col, mixer_col = [piece.reshape(-1) for piece in gathered]
    seq_rows = tokens.shape[0]
    normal_rows = normed(tokens, mixer_gain)

    def fold_one(piece):
        return add_rows(normal_rows, piece)

    outer_sum = fold_one(
        lax.all_gather(outer_weight.astype(jnp.bfloat16), "fs", axis=0, tiled=True)
    )
    inner_sum = fold_one(
        lax.all_gather(inner_weight.astype(jnp.bfloat16), "fs", axis=0, tiled=True)
    )
    value_sum = fold_one(
        lax.all_gather(value_weight.astype(jnp.bfloat16), "fs", axis=0, tiled=True)
    )
    outer = rounded(outer_sum * outer_col)
    inner = rounded(inner_sum * inner_col)
    value = rounded(value_sum * value_col)
    padded = jnp.pad(inner * value, ((2, 0), (0, 0)))
    filtered = (
        filter_taps[0] * padded[0:seq_rows]
        + filter_taps[1] * padded[1 : seq_rows + 1]
        + filter_taps[2] * padded[2:]
    )
    gated = (outer * filtered).astype(jnp.bfloat16)
    mixer_full = lax.all_gather(mixer_weight.astype(jnp.bfloat16), "fs", axis=1, tiled=True)
    return lax.psum_scatter(
        (jnp.dot(gated, mixer_full, preferred_element_type=jnp.float32) * mixer_col).astype(
            jnp.bfloat16
        ),
        "tp",
        scatter_dimension=0,
        tiled=True,
    )


MESH = pl.DeviceIdType.MESH
MATRICES = 3
EARLY = 2
LAG = 2


def mixer_kernel(
    n,
    tokens_hbm,
    gain_hbm,
    w0_hbm,
    w1_hbm,
    w2_hbm,
    taps_hbm,
    w3_hbm,
    s0_hbm,
    s1_hbm,
    s2_hbm,
    s3_hbm,
    out_ref,
    gain_ref,
    taps_ref,
    toks,
    rows,
    stage,
    held,
    mix,
    scales,
    acc,
    product,
    gated,
    gates_in,
    mixed,
    load_sem,
    mixer_sem,
    zl_sem,
    zr_sem,
    zin_sem,
    yout_sem,
    yin_sem,
    dout_sem,
    din_sem,
    small_sem,
    sl_sem,
    sr_sem,
    sin_sem,
    xout_sem,
    xin_sem,
    cout_sem,
    cin_sem,
    rout_sem,
    rin_sem,
    gout_sem,
    gin_sem,
):
    z = lax.axis_index("fs")
    y = lax.axis_index("grp")
    t = lax.axis_index("tp")
    ntp = 4
    block = stage.shape[1]
    half = block // 2
    seq = rows.shape[0]
    tile = seq // ntp
    q = s0_hbm.shape[1]
    pieces = EARLY + n + 1
    last = pieces - 1
    partner = t + 1 - 2 * lax.rem(t, 2)
    across = lax.rem(t + 2, ntp)
    corner = lax.rem(partner + 2, ntp)
    peers = (partner, across, corner)
    weights = (w0_hbm, w1_hbm, w2_hbm)

    barrier = pltpu.get_barrier_semaphore()

    def greet(**target):
        pl.semaphore_signal(barrier, inc=1, device_id=target, device_id_type=MESH)

    @pl.when(z >= 1)
    def _():
        greet(fs=z - 1)

    @pl.when(z <= n - 2)
    def _():
        greet(fs=z + 1)

    for peer in peers:
        greet(tp=peer)
    greet(grp=1 - y)
    at_end = (z == 0) | (z == n - 1)
    greeted = ntp + jnp.where(at_end, 1, 2)

    loads = [
        pltpu.make_async_copy(weights[m], stage.at[m], load_sem.at[m]) for m in range(MATRICES)
    ]

    def mixer_load(i):
        c = lax.rem(EARLY * y + i, n)
        at = pl.ds(pl.multiple_of(c * q, q), q)
        return pltpu.make_async_copy(
            w3_hbm.at[at, :], stage.at[MATRICES, at, :], mixer_sem.at[i]
        )

    def mixer_cast(i):
        mixer_load(i).wait()
        c = lax.rem(EARLY * y + i, n)
        at = pl.ds(pl.multiple_of(c * q, q), q)
        mix[z, c, t] = stage[MATRICES, at, :].astype(jnp.bfloat16)

    token_load = pltpu.make_async_copy(tokens_hbm, toks, load_sem.at[MATRICES])
    small = [
        pltpu.make_async_copy(source, target, small_sem.at[i])
        for i, (source, target) in enumerate(
            (
                (s0_hbm, scales.at[z, :, 0:q]),
                (s1_hbm, scales.at[z, :, q : 2 * q]),
                (s2_hbm, scales.at[z, :, 2 * q : 3 * q]),
                (s3_hbm, scales.at[z, :, 3 * q :]),
                (gain_hbm, gain_ref),
                (taps_hbm, taps_ref),
            )
        )
    ]
    for i in range(EARLY):
        mixer_load(i).start()
    for load in small:
        load.start()
    for i in range(EARLY, n):
        mixer_load(i).start()
    for load in loads + [token_load]:
        load.start()

    def depth_of(p, b):
        c = min(p - EARLY, n - 1)
        if c < n - 1:
            return c, b * block, block
        return c, b * block + (p - EARLY - c) * half, half

    def piece(p, b, side):
        if p < EARLY:
            return mix.at[b, EARLY * side + p, t]
        c, first, count = depth_of(p, b)
        first = pl.multiple_of(first + side * (count // 2), count // 2)
        return held.at[c, pl.ds(first, count // 2), :]

    def remote(ref, send, recv, target):
        return pltpu.make_async_remote_copy(
            src_ref=ref,
            dst_ref=ref,
            send_sem=send,
            recv_sem=recv,
            device_id=target,
            device_id_type=MESH,
        )

    def to_left(p, b):
        return remote(piece(p, b, y), zl_sem.at[p, b], zin_sem.at[p, b], {"fs": z - 1})

    def to_right(p, b):
        return remote(piece(p, b, y), zr_sem.at[p, b], zin_sem.at[p, b], {"fs": z + 1})

    def to_twin(p, b):
        return remote(piece(p, b, y), yout_sem.at[p, b], yin_sem.at[p, b], {"grp": 1 - y})

    def from_twin(p, b):
        return remote(piece(p, b, 1 - y), yout_sem.at[p, b], yin_sem.at[p, b], {"grp": 1 - y})

    inward = jnp.where(z == 0, 1, n - 2)
    outward = jnp.where(z <= 1, 0, n - 1)
    edge = jnp.where(z <= 1, 0, n - 1)

    def second_half(p):
        return remote(piece(p, edge, 1 - y), dout_sem.at[p], din_sem.at[p], {"fs": inward})

    next_in = jnp.where(z <= 1, 1, n - 2)

    def final_half():
        return remote(
            piece(last, next_in, 1 - y), dout_sem.at[pieces], din_sem.at[pieces], {"fs": outward}
        )

    inside = jnp.logical_not(at_end)

    def from_edge(b):
        return inside & (b == edge)

    def from_inside(p, b):
        return at_end & (b == next_in) & (p == last)

    def by_twin(p, b):
        return jnp.logical_not(from_edge(b) | from_inside(p, b))

    def scale_left(b):
        return remote(scales.at[b], sl_sem.at[b], sin_sem.at[b], {"fs": z - 1})

    def scale_right(b):
        return remote(scales.at[b], sr_sem.at[b], sin_sem.at[b], {"fs": z + 1})

    def send_scales():
        @pl.when(z >= 1)
        def _():
            scale_left(z).start()

        @pl.when(z <= n - 2)
        def _():
            scale_right(z).start()

    def relay_scales(s):
        from_right, from_left = z + 1 + s, z - 1 - s

        @pl.when(from_right <= n - 1)
        def _():
            scale_left(from_right).wait_recv()

            @pl.when(z >= 1)
            def _():
                scale_left(from_right).start()

        @pl.when(from_left >= 0)
        def _():
            scale_right(from_left).wait_recv()

            @pl.when(z <= n - 2)
            def _():
                scale_right(from_left).start()

    def send_own(p):
        keep = inside & (p == last)

        @pl.when((z >= 1) & jnp.logical_not(keep & (outward == 0)))
        def _():
            to_left(p, z).start()

        @pl.when((z <= n - 2) & jnp.logical_not(keep & (outward == n - 1)))
        def _():
            to_right(p, z).start()

    def send_final():
        @pl.when(inside & (outward == 0))
        def _():
            to_left(last, z).start()

        @pl.when(inside & (outward == n - 1))
        def _():
            to_right(last, z).start()

        @pl.when(inside)
        def _():
            final_half().start()

    def relay(p, s):
        from_right, from_left = z + 1 + s, z - 1 - s

        @pl.when(from_right <= n - 1)
        def _():
            to_left(p, from_right).wait_recv()

            @pl.when(z >= 1)
            def _():
                to_left(p, from_right).start()

            @pl.when(by_twin(p, from_right))
            def _():
                to_twin(p, from_right).start()

        @pl.when(from_left >= 0)
        def _():
            to_right(p, from_left).wait_recv()

            @pl.when(z <= n - 2)
            def _():
                to_right(p, from_left).start()

            @pl.when(by_twin(p, from_left))
            def _():
                to_twin(p, from_left).start()

    def second_arrived(p, b):
        @pl.when(from_edge(b))
        def _():
            second_half(p).wait_recv()

        if p == last:

            @pl.when(from_inside(p, b))
            def _():
                final_half().wait_recv()

        @pl.when(by_twin(p, b))
        def _():
            from_twin(p, b).wait_recv()

    def each_block(s, act):
        @pl.loop(0, 2)
        def _(side):
            b = z + (1 + s) * (1 - 2 * side)

            @pl.when((b >= 0) & (b <= n - 1))
            def _():
                act(b)

    def across_copy(b):
        return remote(mix.at[b, :, t], xout_sem.at[b], xin_sem.at[b], {"tp": across})

    def across_arrival(b):
        return remote(mix.at[b, :, across], xout_sem.at[b], xin_sem.at[b], {"tp": across})

    def core_copy(b):
        return remote(mix.at[b, :, t], cout_sem.at[b], cin_sem.at[b], {"tp": partner})

    def core_arrival(b):
        return remote(mix.at[b, :, partner], cout_sem.at[b], cin_sem.at[b], {"tp": partner})

    def core_relay(b):
        return remote(mix.at[b, :, across], rout_sem.at[b], rin_sem.at[b], {"tp": partner})

    def core_relay_arrival(b):
        return remote(mix.at[b, :, corner], rout_sem.at[b], rin_sem.at[b], {"tp": partner})

    def spread(b):
        across_copy(b).start()
        core_copy(b).start()

    def spread_arrived(s):
        def act(b):
            for p in range(EARLY):
                second_arrived(p, b)
            spread(b)

        each_block(s, act)

    def pass_on(b):
        across_arrival(b).wait_recv()
        core_relay(b).start()

    def multiply(c, first, count, first_time=False):
        at = pl.ds(pl.multiple_of(first, count), count)
        for i in range(2):
            r = slice(i * seq // 2, (i + 1) * seq // 2)
            part = jnp.dot(rows[r, at], held[c, at, :], preferred_element_type=jnp.float32)
            acc[c, r, :] = part if first_time else acc[c, r, :] + part

    def multiply_arrived(p, s):
        def act(b):
            second_arrived(p, b)
            multiply(*depth_of(p, b))

        each_block(s, act)

    def gate_copy(c, k):
        return pltpu.make_async_remote_copy(
            src_ref=gated.at[c, pl.ds(pl.multiple_of(peers[k] * tile, tile), tile), :],
            dst_ref=gates_in.at[c, t],
            send_sem=gout_sem.at[c, k],
            recv_sem=gin_sem.at[c, k],
            device_id={"tp": peers[k]},
            device_id_type=MESH,
        )

    def gate_arrival(c, k):
        return remote(gates_in.at[c, peers[k]], gout_sem.at[c, k], gin_sem.at[c, k], {"tp": peers[k]})

    def gate(c):
        col = scales[c, :, 0 : 3 * q]
        lanes = slice(c * q, (c + 1) * q)

        def scaled(m):
            part = acc[c, :, m * q : (m + 1) * q] * col[:, m * q : (m + 1) * q]
            return part.astype(jnp.bfloat16).astype(jnp.float32)

        product[8:, :] = scaled(1) * scaled(2)
        filtered = (
            taps_ref[0:1, lanes] * product[6 : 6 + seq, :]
            + taps_ref[1:2, lanes] * product[7 : 7 + seq, :]
            + taps_ref[2:3, lanes] * product[8 : 8 + seq, :]
        )
        gated[c] = (scaled(0) * filtered).astype(jnp.bfloat16)
        for k in (2, 1, 0):
            gate_copy(c, k).start()
        gates_in[c, t] = gated[c, pl.ds(pl.multiple_of(t * tile, tile), tile), :]

    def gates_arrived(c):
        for k in range(ntp - 1):
            gate_arrival(c, k).wait_recv()

    def mix_chunks(first, stop):
        count = stop - first
        left = jnp.concatenate(
            [gates_in[c, k] for c in range(first, stop) for k in range(ntp)], axis=1
        )
        for b in range(n):
            cols = slice(b * block, (b + 1) * block)
            right = mix[b, first:stop].reshape(count * ntp * q, block)
            part = jnp.dot(left, right, preferred_element_type=jnp.float32)
            if first > 0:
                part = mixed[:, cols] + part
            if stop < n:
                mixed[:, cols] = part
            else:
                out_ref[:, cols] = (part * scales[b, :, 3 * q :]).astype(jnp.bfloat16)

    def mix_in():
        @pl.loop(0, n)
        def _(b):
            core_arrival(b).wait_recv()
            core_relay_arrival(b).wait_recv()

    strip = seq // 8

    def normalise(i):
        at = slice(i * strip, (i + 1) * strip)
        rows[at, :] = normed(toks[at, :], gain_ref[...])

    for i in range(EARLY):
        mixer_cast(i)
    pl.semaphore_wait(barrier, greeted)
    send_own(0)
    for load in small:
        load.wait()
    send_scales()
    for p in range(1, EARLY):
        send_own(p)
    for i in range(EARLY, n):
        mixer_cast(i)
    spread(z)
    for m in range(MATRICES):
        loads[m].wait()
        for c in range(n):
            held[c, pl.ds(pl.multiple_of(z * block, block), block), m * q : (m + 1) * q] = stage[
                m, :, c * q : (c + 1) * q
            ].astype(jnp.bfloat16)
    product[0:8, :] = jnp.zeros((8, q), jnp.float32)

    @pl.when(at_end)
    def _():
        for p in range(EARLY):
            second_half(p).start()
        for p in range(EARLY, pieces):
            send_own(p)
            second_half(p).start()

    def send_own_inside(p):
        @pl.when(inside)
        def _():
            send_own(p)

    token_load.wait()

    def own_part(c):
        multiply(c, z * block, block, True)

    part = functools.partial
    hops = n - 1
    order = [(0, 0), (1, 0), (0, 1), (1, 1), (0, 2), (2, 0), (1, 2), (2, 1), (2, 2)]
    order += [(p, s) for p in range(EARLY + 1, last) for s in range(hops)]
    work = {k: [] for k in range(len(order))}
    for i in range(8):
        work[i // 2].append(part(normalise, i))
    for c in range(n):
        work[4 + c // 2].append(part(own_part, c))
    for s in range(hops):
        work[(1, 4, 8)[s]].append(part(relay_scales, s))
        work[order.index((EARLY - 1, s)) + LAG].append(part(spread_arrived, s))
    later = []
    for k, (p, s) in enumerate(order):
        if p >= EARLY:
            tasks = work[k + LAG] if k + LAG < len(order) else later
            tasks.append(part(multiply_arrived, p, s))
            if s == hops - 1 and p - EARLY < n - 1:
                tasks.append(part(gate, p - EARLY))
    work[9].append(lambda: pass_on(z))
    work[13].append(lambda: each_block(0, pass_on))
    work[16].append(lambda: each_block(1, pass_on))
    work[17].append(lambda: each_block(2, pass_on))

    for k, (p, s) in enumerate(order):
        relay(p, s)
        if s == 1 and p != 1:
            send_own_inside(max(p + 1, EARLY))
        for task in work[k]:
            task()

    @pl.when(inside)
    def _():
        relay(last, 0)

    relay(last, 1)
    send_final()
    for task in later:
        task()
    relay(last, 2)
    mix_in()
    for c in range(EARLY):
        gates_arrived(c)
    mix_chunks(0, EARLY)
    multiply_arrived(last, 1)
    multiply_arrived(last, 2)

    @pl.when(at_end)
    def _():
        relay(last, 0)

    multiply_arrived(last, 0)
    gate(n - 1)
    gates_arrived(n - 2)
    mix_chunks(n - 2, n - 1)
    @pl.loop(0, n)
    def _(b):
        across_copy(b).wait_send()
        core_copy(b).wait_send()
        core_relay(b).wait_send()

        @pl.when((b >= z) & (z >= 1))
        def _():
            scale_left(b).wait_send()

        @pl.when((b <= z) & (z <= n - 2))
        def _():
            scale_right(b).wait_send()

    @pl.when(inside)
    def _():
        final_half().wait_send()

    for p in range(pieces):

        @pl.when(at_end)
        def _():
            second_half(p).wait_send()

        @pl.loop(0, n)
        def _(b):
            @pl.when((b >= z) & (z >= 1))
            def _():
                to_left(p, b).wait_send()

            @pl.when((b <= z) & (z <= n - 2))
            def _():
                to_right(p, b).wait_send()

            @pl.when((b != z) & by_twin(p, b))
            def _():
                to_twin(p, b).wait_send()

    gates_arrived(n - 1)
    mix_chunks(n - 1, n)

    for c in range(n):
        for k in range(ntp - 1):
            gate_copy(c, k).wait_send()


def fused_device(
    n,
    tokens,
    mixer_gain,
    outer_weight,
    inner_weight,
    value_weight,
    filter_taps,
    mixer_weight,
    outer_scale,
    inner_scale,
    value_scale,
    mixer_scale,
):
    ntp = 4
    seq, depth = tokens.shape
    block, width = outer_weight.shape
    tile = seq // ntp
    q = outer_scale.shape[1]
    pieces = EARLY + n + 1
    anywhere = pl.BlockSpec(memory_space=pl.ANY)
    bf16, f32 = jnp.bfloat16, jnp.float32
    dma = pltpu.SemaphoreType.DMA
    scale_width = 3 * q + mixer_scale.shape[1]
    return pl.pallas_call(
        functools.partial(mixer_kernel, n),
        out_shape=pltpu.VMEM((tile, n * block), bf16),
        in_specs=[anywhere] * 11,
        out_specs=pl.BlockSpec(memory_space=pltpu.VMEM),
        scratch_shapes=[
            pltpu.VMEM((1, depth), f32),
            pltpu.VMEM(filter_taps.shape, f32),
            pltpu.VMEM((seq, depth), bf16),
            pltpu.VMEM((seq, depth), bf16),
            pltpu.VMEM((MATRICES + 1, block, width), f32),
            pltpu.VMEM((n, depth, MATRICES * q), bf16),
            pltpu.VMEM((n, n, ntp, q, block), bf16),
            pltpu.VMEM((n, 1, scale_width), f32),
            pltpu.VMEM((n, seq, MATRICES * q), f32),
            pltpu.VMEM((seq + 8, q), f32),
            pltpu.VMEM((n, seq, q), bf16),
            pltpu.VMEM((n, ntp, tile, q), bf16),
            pltpu.VMEM((tile, n * block), f32),
            dma((MATRICES + 1,)),
            dma((n,)),
            dma((pieces, n)),
            dma((pieces, n)),
            dma((pieces, n)),
            dma((pieces, n)),
            dma((pieces, n)),
            dma((pieces + 1,)),
            dma((pieces + 1,)),
            dma((6,)),
            dma((n,)),
            dma((n,)),
            dma((n,)),
            dma((n,)),
            dma((n,)),
            dma((n,)),
            dma((n,)),
            dma((n,)),
            dma((n,)),
            dma((n, ntp - 1)),
            dma((n, ntp - 1)),
        ],
        compiler_params=pltpu.CompilerParams(
            collective_id=0, has_side_effects=True, vmem_limit_bytes=60 * 2**20
        ),
    )(
        tokens,
        mixer_gain.reshape(1, -1),
        outer_weight,
        inner_weight,
        value_weight,
        filter_taps,
        mixer_weight,
        outer_scale,
        inner_scale,
        value_scale,
        mixer_scale,
    )


def choose(mesh):
    n, ntp, groups = mesh.shape["fs"], mesh.shape["tp"], mesh.shape["grp"]

    def run(*args):
        tokens, weight, mixer, scale = args[0], args[2], args[6], args[7]
        fits = (
            groups == 2
            and ntp == 4
            and n == 4
            and weight.shape == mixer.shape
            and weight.shape[0] == n * scale.shape[1]
            and scale.shape[1] % 128 == 0
            and tokens.shape[0] % 256 == 0
        )
        return fused_device(n, *args) if fits else per_device(*args)

    return run


def solution(mesh):
    in_specs = (
        P(("grp", "fs"), None),
        P(),
        P("fs", "tp"),
        P("fs", "tp"),
        P("fs", "tp"),
        P(None, "tp"),
        P("tp", "fs"),
        P("tp", "fs"),
        P("tp", "fs"),
        P("tp", "fs"),
        P(None, "fs"),
    )
    out_specs = P(("grp", "fs", "tp"), None)
    return jax.shard_map(
        choose(mesh), mesh=mesh, in_specs=in_specs, out_specs=out_specs, check_vma=False
    )
```
